32 devices in a mesh: grp: 2 (over y), fs: 4 (over z), tp: 4 (over x, core).
Axes of the slice: x: 2, y: 2, z: 4, core: 2. Of those that a mesh axis runs over, the one named last changes fastest.
Arguments:
- tokens: bfloat16 [4096, 2048], P(('grp', 'fs')), parts along dimension 0, may hold values from -6 to 6
- pre_gain: float32 [2048], replicated, may hold values from 0.1 to 1.9
- up_weight: float32 [2048, 8192], P('fs', 'tp'), may hold values from -0.125 to 0.125
- up_scale: float32 [8192], P('tp'), may hold values from 0.3 to 3
- down_weight: float32 [8192, 2048], P('tp', 'fs'), may hold values from -0.0625 to 0.0625
- down_scale: float32 [2048], P('fs'), may hold values from 0.3 to 3
- post_gain: float32 [2048], replicated, may hold values from 0.1 to 1.9
Outputs:
- mixed: bfloat16 [4096, 2048], P(('grp', 'fs')), parts along dimension 0
The draws below stay inside these ranges and needn't reach their ends.
There are 2 independent parts, one for each index of `grp`. The reference program is written for one: setup_inputs(seed, part) draws one part's arguments, and reference() takes and returns one part's arrays. A program takes and returns all parts, laid end to end along the dimension named above; an argument that names none is the same for every part. Nothing has to cross between parts.
All inputs are finite; a program needn't handle non-finite values.
Results may differ from the reference program's by a relative error of at most 0.01.
Values may be sent and summed in bfloat16 or wider, within the bound.
A program may use at most 64 MiB of HBM per device.

```python
import math
import jax
import jax.numpy as jnp
from jax import lax

D = 2048
FF = 8192
TOK_DEV = 512
TOKENS = 2048
N_FS = 4
N_TP = 4


def levels(rng, shape, cuts, least, top_value):
    def one(dim, blocks):
        steps = jax.random.uniform(jax.random.fold_in(jax.random.fold_in(rng, 6), dim), (blocks,), jnp.float32, least / len(cuts), top_value / len(cuts))
        return jnp.repeat(jnp.exp(steps), shape[dim] // blocks).reshape((-1,) + (1,) * (len(shape) - dim - 1))

    gain = one(*cuts[0])
    for cut in cuts[1:]:
        gain = gain * one(*cut)
    return gain


def scatter_about(key, shape, scale, limit, split=(), dtype=jnp.bfloat16):
    gain = levels(key, shape, split, -0.22, 0.18) if split else 1.0
    values = jax.random.normal(key, shape, jnp.float32) * scale * gain
    return jnp.minimum(jnp.maximum(values, -limit), limit).astype(dtype)


def setup_inputs(seed: int = 0, part: int = 0) -> dict:
    seeds = jax.random.split(jax.random.key(seed), 8)
    part_keys = jax.random.split(jax.random.fold_in(seeds[7], part), 8)
    tokens = scatter_about(part_keys[0], (TOKENS, D), 1.0, 6.0, ((0, 4),))
    pre_gain = jnp.clip(1.0 + 0.18 * jax.random.normal(seeds[1], (D,), jnp.float32), 0.1, 1.9)
    up_weight = scatter_about(seeds[2], (D, FF), D ** -0.5, 0.125, ((0, 4), (1, 4)), jnp.float32)
    up_scale = jnp.clip(jnp.exp(math.log(3.0) - 2.3025851 * jax.random.uniform(seeds[3], (FF,), jnp.float32) ** levels(seeds[3], (FF,), ((0, 4),), -0.2, 0.2)), 0.3, 3.0)
    down_weight = scatter_about(seeds[4], (FF, D), FF ** -0.5, 0.0625, ((0, 4), (1, 4)), jnp.float32)
    down_scale = jnp.clip(jnp.exp(math.log(3.0) - 2.3025851 * jax.random.uniform(seeds[5], (D,), jnp.float32) ** levels(seeds[5], (D,), ((0, 4),), -0.2, 0.2)), 0.3, 3.0)
    post_gain = jnp.clip(1.0 + 0.18 * jax.random.normal(seeds[6], (D,), jnp.float32), 0.1, 1.9)
    return {"tokens": tokens, "pre_gain": pre_gain, "up_weight": up_weight, "up_scale": up_scale, "down_weight": down_weight, "down_scale": down_scale, "post_gain": post_gain}


epsilon = 1e-06

def rms_rows(values, scaling):
    return values * lax.rsqrt(lax.optimization_barrier(jnp.mean(values * values, axis=-1, keepdims=True)) + epsilon) * scaling

def reference(tokens, pre_gain, up_weight, up_scale, down_weight, down_scale, post_gain):
    up_cast = up_weight.astype(jnp.bfloat16)
    down_cast = down_weight.astype(jnp.bfloat16)
    block_width = FF // N_TP

    def row_block(rows):
        residual = rows.astype(jnp.float32)
        normed = rms_rows(residual, pre_gain).astype(jnp.bfloat16)
        lifted = jnp.dot(normed, up_cast, preferred_element_type=jnp.float32) * up_scale
        hidden = jnp.square(jax.nn.relu(lifted)).astype(jnp.bfloat16)
        running = jnp.zeros((rows.shape[0], D), jnp.float32)
        for member in range(N_TP):
            low = member * block_width
            high = low + block_width
            partial_value = jnp.dot(hidden[:, low:high], down_cast[low:high], preferred_element_type=jnp.float32) * down_scale
            partial_value = lax.optimization_barrier(partial_value.astype(jnp.bfloat16))
            running = running + partial_value.astype(jnp.float32)
        branch = lax.optimization_barrier(running.astype(jnp.bfloat16)).astype(jnp.float32)
        return (residual + rms_rows(branch, post_gain)).astype(jnp.bfloat16)
    result = lax.map(row_block, tokens.reshape(N_FS, TOK_DEV, D))
    return result.reshape(N_FS * TOK_DEV, D)
```

```python
import functools

import jax
import jax.numpy as jnp
from jax import lax
from jax.experimental import pallas as pl
from jax.experimental.pallas import tpu as pltpu
from jax.sharding import PartitionSpec as P

epsilon = 1e-06
MESH = pl.DeviceIdType.MESH
CHUNKS = 2


def rms_rows(values, scaling):
    return values * lax.rsqrt(jnp.mean(values * values, axis=-1, keepdims=True) + epsilon) * scaling


def activate(lifted, up_scale):
    return jnp.square(jax.nn.relu(lifted * up_scale)).astype(jnp.bfloat16)


def plain(tokens, pre_gain, up_weight, up_scale, down_weight, down_scale, post_gain):
    residual = tokens.astype(jnp.float32)
    normed = rms_rows(residual, pre_gain).astype(jnp.bfloat16)
    up_cast = up_weight.astype(jnp.bfloat16)
    down_cast = down_weight.astype(jnp.bfloat16)
    column_scales = lax.all_gather(down_scale, "fs", axis=0, tiled=True)
    up_full, down_full = (
        lax.all_gather(up_cast, "fs", axis=0, tiled=True),
        lax.all_gather(down_cast, "fs", axis=1, tiled=True),
    )
    lifted = jnp.dot(normed, up_full, preferred_element_type=jnp.float32)
    hidden = activate(lifted, up_scale)
    partials = jnp.dot(hidden, down_full, preferred_element_type=jnp.float32)
    partials = (partials * column_scales).astype(jnp.bfloat16)
    summed = lax.psum(partials, "tp").astype(jnp.float32)
    branch = lax.optimization_barrier(summed.astype(jnp.bfloat16)).astype(jnp.float32)
    return (residual + rms_rows(branch, post_gain)).astype(jnp.bfloat16)


def kernel(nc, normed, up_in, down_in, up_scale, down_scale, out, up, down, tok, hid, scl, keep, core_out, core_in,
           x_out, x_in, branch, ship, send, wrecv, tok_recv, scl_recv, core_recv, x_recv, br_recv, local):
    g, z, t = lax.axis_index("grp"), lax.axis_index("fs"), lax.axis_index("tp")
    core, x = lax.rem(t, 2), t // 2
    pair = z // 2
    outer, inner, other = 3 * pair, 1 + pair, 2 - pair
    outer2 = 3 - outer
    is_outer = z == outer
    n_tp = 4
    rows = normed.shape[0]
    depth, half = up_in.shape[1], up_in.shape[2]
    du, dc = depth // nc, down_in.shape[2]
    quarter = rows // n_tp
    core_peer, x_peer = x * 2 + 1 - core, (1 - x) * 2 + core

    barrier = pltpu.get_barrier_semaphore()
    peers = [{"fs": lax.rem(z + o, 4)} for o in range(1, 4)] + [{"grp": 1 - g}]
    peers += [{"tp": lax.rem(t + o, n_tp)} for o in range(1, n_tp)]
    for peer in peers:
        pl.semaphore_signal(barrier, inc=1, device_id=peer, device_id_type=MESH)
    pl.semaphore_wait(barrier, len(peers))

    def remote(src, dst, s, r, peer):
        return pltpu.make_async_remote_copy(src_ref=src, dst_ref=dst, send_sem=send.at[s], recv_sem=r,
                                            device_id=peer, device_id_type=MESH)

    def up_slot(zz, c, h):
        return up.at[h, pl.ds(pl.multiple_of(zz * depth + c * du, du), du), :]

    def down_slot(zz, c, h):
        return down.at[zz * nc + c, pl.ds(pl.multiple_of(h * half, half), half), :]

    def up_src(c, h):
        return up_in.at[h, pl.ds(c * du, du), :]

    def down_src(c, h):
        return down_in.at[c, pl.ds(pl.multiple_of(h * half, half), half), :]

    slots, sources = (up_slot, down_slot), (up_src, down_src)

    def tok_slot(n, q):
        return tok.at[pl.ds(pl.multiple_of(n * rows + q * quarter, quarter), quarter), :]

    def weight(kind, src, zz, c, h, s, peer):
        return remote(src, slots[kind](zz, c, h), s, wrecv.at[kind, zz, c, h], peer)

    def arrived(kind, zz, c, h):
        slot = slots[kind](zz, c, h)
        weight(kind, slot, zz, c, h, 0, {"fs": z}).wait_recv()

    def block(b):
        return branch.at[b]

    @pl.when(is_outer)
    def _():
        started = []
        to = {"fs": inner}

        def go(copy):
            copy.start()
            started.append(copy)

        go(remote(down_scale, scl.at[z], 0, scl_recv.at[z], to))
        go(remote(down_scale, scl.at[z], 1, scl_recv.at[z], {"fs": other}))
        for c in range(nc):
            go(weight(0, up_src(c, g), z, c, g, 2 + c, to))
        mine = normed.at[pl.ds(pl.multiple_of(t * quarter, quarter), quarter), :]
        go(remote(mine, tok_slot(1, t), 2 + nc, tok_recv.at[t], to))
        for c in range(nc):
            go(weight(0, up_src(c, 1 - g), z, c, 1 - g, 3 + nc + c, to))
        for c in range(nc):
            go(weight(1, down_src(c, g), z, c, g, 3 + 2 * nc + c, to))
        for c in range(nc):
            go(weight(1, down_src(c, 1 - g), z, c, 1 - g, 3 + 3 * nc + c, to))
        for copy in started:
            copy.wait_send()
        for b in range(4 * nc):
            remote(block(b), block(b), 0, br_recv.at[b], to).wait_recv()

    @pl.when(jnp.logical_not(is_outer))
    def _():
        started = []
        counter = [0]

        def fresh():
            counter[0] += 1
            return counter[0] - 1

        def go(copy):
            copy.start()
            started.append(copy)

        across, beside = {"fs": other}, {"grp": 1 - g}
        for c in range(nc):
            go(weight(0, up_src(c, g), z, c, g, fresh(), across))
        go(remote(down_scale, scl.at[z], fresh(), scl_recv.at[z], across))
        locals_ = [
            pltpu.make_async_copy(normed, tok.at[pl.ds(0, rows), :], local.at[0]),
            pltpu.make_async_copy(down_scale, scl.at[z], local.at[1]),
        ]
        for h in range(2):
            locals_.append(pltpu.make_async_copy(
                up_in.at[h], up.at[h, pl.ds(pl.multiple_of(z * depth, depth), depth), :], local.at[2 + h]))
        for c in range(nc):
            locals_.append(pltpu.make_async_copy(down_in.at[c], down.at[z * nc + c], local.at[4 + c]))
        for copy in locals_:
            copy.start()

        def forward(kind, c):
            arrived(kind, outer, c, g)
            go(weight(kind, slots[kind](outer, c, g), outer, c, g, fresh(), across))

        def relay(kind, zz, c):
            arrived(kind, zz, c, g)
            go(weight(kind, slots[kind](zz, c, g), zz, c, g, fresh(), beside))

        for c in range(nc):
            forward(0, c)
            relay(0, other, c)
        for c in range(nc):
            go(weight(1, down_src(c, g), z, c, g, fresh(), across))
        remote(tok_slot(1, t), tok_slot(1, t), 0, tok_recv.at[t], {"fs": outer}).wait_recv()
        for o in range(1, n_tp):
            go(remote(tok_slot(1, t), tok_slot(1, t), fresh(), tok_recv.at[t], {"tp": lax.rem(t + o, n_tp)}))
        for copy in locals_:
            copy.wait()
        for c in range(nc):
            relay(0, outer2, c)
        for o in range(1, n_tp):
            q = lax.rem(t + o, n_tp)
            remote(tok_slot(1, q), tok_slot(1, q), 0, tok_recv.at[q], {"tp": q}).wait_recv()

        tile = dc

        def lift(h):
            def one(i, _):
                columns = pl.ds(pl.multiple_of(i * tile, tile), tile)
                whole = pl.ds(pl.multiple_of(h * half + i * tile, tile), tile)
                for n in range(2):
                    part = pl.ds(n * rows, rows)
                    lifted = jnp.dot(tok[part, :], up[h, :, columns], preferred_element_type=jnp.float32)
                    hid[part, whole] = activate(lifted, up_scale[:, whole])
                return 0
            lax.fori_loop(0, half // tile, one, 0)

        lift(g)
        relay(1, other, 0)
        for c in range(nc):
            arrived(0, outer, c, 1 - g)
            arrived(0, other, c, 1 - g)
            arrived(0, outer2, c, 1 - g)
        lift(1 - g)
        for c in range(1, nc):
            relay(1, other, c)

        def project(zz, c):
            b = zz * nc + c
            theirs = jnp.dot(hid[pl.ds(pl.multiple_of((1 - core) * rows, rows), rows), :], down[b],
                             preferred_element_type=jnp.float32)
            core_out[b] = theirs.astype(jnp.bfloat16)
            go(remote(core_out.at[b], core_in.at[b], fresh(), core_recv.at[b], {"tp": core_peer}))
            keep[lax.rem(b, 2)] = jnp.dot(hid[pl.ds(pl.multiple_of(core * rows, rows), rows), :], down[b],
                              preferred_element_type=jnp.float32)

        def cross(zz, c):
            b = zz * nc + c
            remote(core_out.at[b], core_in.at[b], 0, core_recv.at[b], {"tp": core_peer}).wait_recv()
            x_out[b] = (keep[lax.rem(b, 2)] + core_in[b].astype(jnp.float32)).astype(jnp.bfloat16)
            go(remote(x_out.at[b], x_in.at[b], fresh(), x_recv.at[b], {"tp": x_peer}))

        last = []
        for _ in range(4 * nc):
            last.append((fresh(), fresh()))

        def finish(i, zz, c):
            b = zz * nc + c
            remote(x_out.at[b], x_in.at[b], 0, x_recv.at[b], {"tp": x_peer}).wait_recv()
            total = x_out[b].astype(jnp.float32) + x_in[b].astype(jnp.float32)
            value = (total * scl[zz, :, pl.ds(c * dc, dc)]).astype(jnp.bfloat16)

            @pl.when(core == 0)
            def _():
                branch[b] = value
                remote(block(b), block(b), last[i][0], br_recv.at[b], {"tp": core_peer}).start()

            @pl.when(core == 1)
            def _():
                ship[b] = value
                for k in range(2):
                    remote(ship.at[b], block(b), last[i][k], br_recv.at[b], {"fs": outer, "tp": x * 2 + k}).start()

        for zz in (outer, other, outer2):
            remote(down_scale, scl.at[zz], 0, scl_recv.at[zz], {"fs": zz}).wait_recv()

        order = [(z, c) for c in range(nc)] + [(other, c) for c in range(nc)]
        for c in range(nc):
            order += [(outer2, c), (outer, c)]
        n = len(order)
        for i in range(n + 2):
            if i < n:
                zz, c = order[i]
                if i >= nc:
                    arrived(1, zz, c, 1 - g)
                project_now = True
            else:
                project_now = False
            if 0 <= i - 1 < n:
                cross(*order[i - 1])
            if project_now:
                project(*order[i])
            if 0 <= i - 2 < n:
                finish(i - 2, *order[i - 2])
            if i < nc:
                forward(1, i)
            elif i < 2 * nc:
                relay(1, outer2, i - nc)
        for copy in started:
            copy.wait_send()
        for i, (zz, c) in enumerate(order):
            b = zz * nc + c

            @pl.when(core == 0)
            def _():
                remote(block(b), block(b), last[i][0], br_recv.at[b], {"tp": core_peer}).wait_send()

            @pl.when(core == 1)
            def _():
                for k in range(2):
                    remote(ship.at[b], block(b), last[i][k], br_recv.at[b], {"fs": outer, "tp": x * 2 + k}).wait_send()
                remote(block(b), block(b), last[i][0], br_recv.at[b], {"tp": core_peer}).wait_recv()

    for b in range(4 * nc):
        out[:, b * dc:(b + 1) * dc] = branch[b]


def fused(tokens, pre_gain, up_weight, up_scale, down_weight, down_scale, post_gain):
    nc = CHUNKS
    rows, width = tokens.shape
    depth, ff = up_weight.shape
    half, dc = ff // 2, depth // nc
    residual = tokens.astype(jnp.float32)
    normed = rms_rows(residual, pre_gain).astype(jnp.bfloat16)
    up_in = up_weight.astype(jnp.bfloat16).reshape(depth, 2, half).transpose(1, 0, 2)
    down_in = down_weight.astype(jnp.bfloat16).reshape(ff, nc, dc).transpose(1, 0, 2)
    blocks = 4 * nc
    bf, f32 = jnp.bfloat16, jnp.float32
    dma = pltpu.SemaphoreType.DMA
    anywhere, vmem = pl.BlockSpec(memory_space=pl.ANY), pl.BlockSpec(memory_space=pltpu.VMEM)
    branch = pl.pallas_call(
        functools.partial(kernel, nc),
        out_shape=jax.ShapeDtypeStruct((rows, width), bf),
        in_specs=[anywhere, anywhere, anywhere, vmem, vmem],
        out_specs=vmem,
        scratch_shapes=[
            pltpu.VMEM((2, width, half), bf),
            pltpu.VMEM((blocks, ff, dc), bf),
            pltpu.VMEM((2 * rows, width), bf),
            pltpu.VMEM((2 * rows, ff), bf),
            pltpu.VMEM((4, 1, depth), f32),
            pltpu.VMEM((2, rows, dc), f32),
            pltpu.VMEM((blocks, rows, dc), bf),
            pltpu.VMEM((blocks, rows, dc), bf),
            pltpu.VMEM((blocks, rows, dc), bf),
            pltpu.VMEM((blocks, rows, dc), bf),
            pltpu.VMEM((blocks, rows, dc), bf),
            pltpu.VMEM((blocks, rows, dc), bf),
            dma((64 * nc,)),
            dma((2, 4, nc, 2)),
            dma((4,)),
            dma((4,)),
            dma((blocks,)),
            dma((blocks,)),
            dma((blocks,)),
            dma((4 + nc,)),
        ],
        compiler_params=pltpu.CompilerParams(
            collective_id=0, has_side_effects=True, vmem_limit_bytes=60 << 20
        ),
    )(normed, up_in, down_in, up_scale.reshape(1, ff), down_scale.reshape(1, depth))
    branch = branch.astype(jnp.float32)
    return (residual + rms_rows(branch, post_gain)).astype(jnp.bfloat16)


def solution(mesh):
    placed = (P(("grp", "fs"), None), P(), P("fs", "tp"), P("tp"), P("tp", "fs"), P("fs"), P())
    sizes = mesh.shape
    line = sizes["grp"] == 2 and sizes["fs"] == 4 and sizes["tp"] == 4
    return jax.shard_map(
        fused if line else plain, mesh=mesh, in_specs=placed, out_specs=P(("grp", "fs"), None), check_vma=False
    )
```

```python
import functools

import jax
import jax.numpy as jnp
from jax import lax
from jax.experimental import pallas as pl
from jax.experimental.pallas import tpu as pltpu
from jax.sharding import PartitionSpec as P

epsilon = 1e-06
MESH = pl.DeviceIdType.MESH
CHUNKS = 2


def rms_rows(values, scaling):
    return values * lax.rsqrt(jnp.mean(values * values, axis=-1, keepdims=True) + epsilon) * scaling


def activate(lifted, up_scale):
    return jnp.square(jax.nn.relu(lifted * up_scale)).astype(jnp.bfloat16)


def plain(tokens, pre_gain, up_weight, up_scale, down_weight, down_scale, post_gain):
    residual = tokens.astype(jnp.float32)
    normed = rms_rows(residual, pre_gain).astype(jnp.bfloat16)
    up_cast = up_weight.astype(jnp.bfloat16)
    down_cast = down_weight.astype(jnp.bfloat16)
    column_scales = lax.all_gather(down_scale, "fs", axis=0, tiled=True)
    up_full, down_full = (
        lax.all_gather(up_cast, "fs", axis=0, tiled=True),
        lax.all_gather(down_cast, "fs", axis=1, tiled=True),
    )
    lifted = jnp.dot(normed, up_full, preferred_element_type=jnp.float32)
    hidden = activate(lifted, up_scale)
    partials = jnp.dot(hidden, down_full, preferred_element_type=jnp.float32)
    partials = (partials * column_scales).astype(jnp.bfloat16)
    summed = lax.psum(partials, "tp").astype(jnp.float32)
    branch = lax.optimization_barrier(summed.astype(jnp.bfloat16)).astype(jnp.float32)
    return (residual + rms_rows(branch, post_gain)).astype(jnp.bfloat16)


def kernel(nc, tokens, up_in, down_in, up_scale, down_scale, pre_gain, post_gain, out, res, up_f32, down_f32, up,
           down, tok, hid, scl, keep, core_out, core_in,
           x_out, x_in, branch, ship, send, wrecv, tok_recv, scl_recv, core_recv, x_recv, br_recv, local, one_sem):
    g, z, t = lax.axis_index("grp"), lax.axis_index("fs"), lax.axis_index("tp")
    core, x = lax.rem(t, 2), t // 2
    pair = z // 2
    outer, inner, other = 3 * pair, 1 + pair, 2 - pair
    outer2 = 3 - outer
    is_outer = z == outer
    n_tp = 4
    rows = tokens.shape[0]
    depth, half = up_in.shape[0], up_in.shape[1] // 2
    du, dc = depth // nc, depth // nc
    quarter = rows // n_tp
    core_peer, x_peer = x * 2 + 1 - core, (1 - x) * 2 + core

    def at_half(h):
        return pl.ds(pl.multiple_of(h * half, half), half)

    def load(kind, c, h):
        if kind == 0:
            place = pl.ds(c * du, du), at_half(h)
            pair = up_in.at[place], up_f32.at[place]
        else:
            place = at_half(h), pl.ds(c * dc, dc)
            pair = down_in.at[place], down_f32.at[place]
        return pltpu.make_async_copy(*pair, local.at[kind, c, h])

    for c in range(nc):
        load(0, c, g).start()
    fetch = pltpu.make_async_copy(tokens, res, one_sem.at[0])
    fetch.start()
    for c in range(nc):
        load(0, c, 1 - g).start()
    for h in (g, 1 - g):
        for c in range(nc):
            load(1, c, h).start()

    barrier = pltpu.get_barrier_semaphore()
    peers = [{"fs": lax.rem(z + o, 4)} for o in range(1, 4)] + [{"grp": 1 - g}]
    peers += [{"tp": lax.rem(t + o, n_tp)} for o in range(1, n_tp)]
    for peer in peers:
        pl.semaphore_signal(barrier, inc=1, device_id=peer, device_id_type=MESH)
    pl.semaphore_wait(barrier, len(peers))

    def remote(src, dst, s, r, peer):
        return pltpu.make_async_remote_copy(src_ref=src, dst_ref=dst, send_sem=send.at[s], recv_sem=r,
                                            device_id=peer, device_id_type=MESH)

    def up_slot(zz, c, h):
        return up.at[h, pl.ds(pl.multiple_of(zz * depth + c * du, du), du), :]

    def down_slot(zz, c, h):
        return down.at[zz * nc + c, pl.ds(pl.multiple_of(h * half, half), half), :]

    slots = (up_slot, down_slot)

    def cast(kind, c, h):
        load(kind, c, h).wait()
        if kind == 0:
            up[h, pl.ds(pl.multiple_of(z * depth + c * du, du), du), :] = up_f32[
                pl.ds(c * du, du), at_half(h)].astype(jnp.bfloat16)
        else:
            down[z * nc + c, at_half(h), :] = down_f32[at_half(h), pl.ds(c * dc, dc)].astype(jnp.bfloat16)

    def norm_rows(first, n, step):
        def one(i, _):
            part = pl.ds(pl.multiple_of(first + i * step, step), step)
            tok[part, :] = rms_rows(res[part, :].astype(jnp.float32), pre_gain[...]).astype(jnp.bfloat16)
            return 0
        lax.fori_loop(0, n // step, one, 0)

    def tok_slot(n, q):
        return tok.at[pl.ds(pl.multiple_of(n * rows + q * quarter, quarter), quarter), :]

    def weight(kind, src, zz, c, h, s, peer):
        return remote(src, slots[kind](zz, c, h), s, wrecv.at[kind, zz, c, h], peer)

    def arrived(kind, zz, c, h):
        slot = slots[kind](zz, c, h)
        weight(kind, slot, zz, c, h, 0, {"fs": z}).wait_recv()

    def block(b):
        return branch.at[b]

    @pl.when(is_outer)
    def _():
        started = []
        to = {"fs": inner}

        def go(copy):
            copy.start()
            started.append(copy)

        go(remote(down_scale, scl.at[z], 0, scl_recv.at[z], to))
        go(remote(down_scale, scl.at[z], 1, scl_recv.at[z], {"fs": other}))
        for c in range(nc):
            cast(0, c, g)
            go(weight(0, up_slot(z, c, g), z, c, g, 2 + c, to))
        fetch.wait()
        norm_rows(t * quarter, quarter, min(quarter, 64))
        go(remote(tok_slot(0, t), tok_slot(1, t), 2 + nc, tok_recv.at[t], to))
        for c in range(nc):
            cast(0, c, 1 - g)
            go(weight(0, up_slot(z, c, 1 - g), z, c, 1 - g, 3 + nc + c, to))
        for c in range(nc):
            cast(1, c, g)
            go(weight(1, down_slot(z, c, g), z, c, g, 3 + 2 * nc + c, to))
        for c in range(nc):
            cast(1, c, 1 - g)
            go(weight(1, down_slot(z, c, 1 - g), z, c, 1 - g, 3 + 3 * nc + c, to))
        for copy in started:
            copy.wait_send()
        for b in range(4 * nc):
            remote(block(b), block(b), 0, br_recv.at[b], to).wait_recv()

    @pl.when(jnp.logical_not(is_outer))
    def _():
        started = []
        counter = [0]

        def fresh():
            counter[0] += 1
            return counter[0] - 1

        def go(copy):
            copy.start()
            started.append(copy)

        across, beside = {"fs": other}, {"grp": 1 - g}
        for c in range(nc):
            cast(0, c, g)
            go(weight(0, up_slot(z, c, g), z, c, g, fresh(), across))
        go(remote(down_scale, scl.at[z], fresh(), scl_recv.at[z], across))
        own_scale = pltpu.make_async_copy(down_scale, scl.at[z], one_sem.at[1])
        own_scale.start()
        for c in range(nc):
            cast(1, c, g)
        fetch.wait()
        norm_rows(0, rows, 64)
        own_scale.wait()

        def forward(kind, c):
            arrived(kind, outer, c, g)
            go(weight(kind, slots[kind](outer, c, g), outer, c, g, fresh(), across))

        def relay(kind, zz, c):
            arrived(kind, zz, c, g)
            go(weight(kind, slots[kind](zz, c, g), zz, c, g, fresh(), beside))

        for c in range(nc):
            forward(0, c)
            relay(0, other, c)
        for c in range(nc):
            go(weight(1, down_slot(z, c, g), z, c, g, fresh(), across))
        remote(tok_slot(1, t), tok_slot(1, t), 0, tok_recv.at[t], {"fs": outer}).wait_recv()
        for o in range(1, n_tp):
            go(remote(tok_slot(1, t), tok_slot(1, t), fresh(), tok_recv.at[t], {"tp": lax.rem(t + o, n_tp)}))
        for c in range(nc):
            cast(0, c, 1 - g)
        for c in range(nc):
            cast(1, c, 1 - g)
        for c in range(nc):
            relay(0, outer2, c)
        for o in range(1, n_tp):
            q = lax.rem(t + o, n_tp)
            remote(tok_slot(1, q), tok_slot(1, q), 0, tok_recv.at[q], {"tp": q}).wait_recv()

        tile = dc

        def lift(h):
            def one(i, _):
                columns = pl.ds(pl.multiple_of(i * tile, tile), tile)
                whole = pl.ds(pl.multiple_of(h * half + i * tile, tile), tile)
                for n in range(2):
                    part = pl.ds(n * rows, rows)
                    lifted = jnp.dot(tok[part, :], up[h, :, columns], preferred_element_type=jnp.float32)
                    hid[part, whole] = activate(lifted, up_scale[:, whole])
                return 0
            lax.fori_loop(0, half // tile, one, 0)

        lift(g)
        relay(1, other, 0)
        for c in range(nc):
            arrived(0, outer, c, 1 - g)
            arrived(0, other, c, 1 - g)
            arrived(0, outer2, c, 1 - g)
        lift(1 - g)
        for c in range(1, nc):
            relay(1, other, c)

        def project(zz, c):
            b = zz * nc + c
            theirs = jnp.dot(hid[pl.ds(pl.multiple_of((1 - core) * rows, rows), rows), :], down[b],
                             preferred_element_type=jnp.float32)
            core_out[b] = theirs.astype(jnp.bfloat16)
            go(remote(core_out.at[b], core_in.at[b], fresh(), core_recv.at[b], {"tp": core_peer}))
            keep[lax.rem(b, 2)] = jnp.dot(hid[pl.ds(pl.multiple_of(core * rows, rows), rows), :], down[b],
                              preferred_element_type=jnp.float32)

        def cross(zz, c):
            b = zz * nc + c
            remote(core_out.at[b], core_in.at[b], 0, core_recv.at[b], {"tp": core_peer}).wait_recv()
            x_out[b] = (keep[lax.rem(b, 2)] + core_in[b].astype(jnp.float32)).astype(jnp.bfloat16)
            go(remote(x_out.at[b], x_in.at[b], fresh(), x_recv.at[b], {"tp": x_peer}))

        last = []
        for _ in range(4 * nc):
            last.append((fresh(), fresh()))

        def finish(i, zz, c):
            b = zz * nc + c
            remote(x_out.at[b], x_in.at[b], 0, x_recv.at[b], {"tp": x_peer}).wait_recv()
            total = x_out[b].astype(jnp.float32) + x_in[b].astype(jnp.float32)
            value = (total * scl[zz, :, pl.ds(c * dc, dc)]).astype(jnp.bfloat16)

            @pl.when(core == 0)
            def _():
                branch[b] = value
                remote(block(b), block(b), last[i][0], br_recv.at[b], {"tp": core_peer}).start()

            @pl.when(core == 1)
            def _():
                ship[b] = value
                for k in range(2):
                    remote(ship.at[b], block(b), last[i][k], br_recv.at[b], {"fs": outer, "tp": x * 2 + k}).start()

        for zz in (outer, other, outer2):
            remote(down_scale, scl.at[zz], 0, scl_recv.at[zz], {"fs": zz}).wait_recv()

        order = [(z, c) for c in range(nc)] + [(other, c) for c in range(nc)]
        for c in range(nc):
            order += [(outer2, c), (outer, c)]
        n = len(order)
        for i in range(n + 2):
            if i < n:
                zz, c = order[i]
                if i >= nc:
                    arrived(1, zz, c, 1 - g)
                project_now = True
            else:
                project_now = False
            if 0 <= i - 1 < n:
                cross(*order[i - 1])
            if project_now:
                project(*order[i])
            if 0 <= i - 2 < n:
                finish(i - 2, *order[i - 2])
            if i < nc:
                forward(1, i)
            elif i < 2 * nc:
                relay(1, outer2, i - nc)
        for copy in started:
            copy.wait_send()
        for i, (zz, c) in enumerate(order):
            b = zz * nc + c

            @pl.when(core == 0)
            def _():
                remote(block(b), block(b), last[i][0], br_recv.at[b], {"tp": core_peer}).wait_send()

            @pl.when(core == 1)
            def _():
                for k in range(2):
                    remote(ship.at[b], block(b), last[i][k], br_recv.at[b], {"fs": outer, "tp": x * 2 + k}).wait_send()
                remote(block(b), block(b), last[i][0], br_recv.at[b], {"tp": core_peer}).wait_recv()

    def close(i, _):
        part = pl.ds(pl.multiple_of(i * 64, 64), 64)
        row = jnp.concatenate([branch[b, part, :] for b in range(4 * nc)], axis=1).astype(jnp.float32)
        out[part, :] = (res[part, :].astype(jnp.float32) + rms_rows(row, post_gain[...])).astype(jnp.bfloat16)
        return 0

    lax.fori_loop(0, rows // 64, close, 0)


def fused(tokens, pre_gain, up_weight, up_scale, down_weight, down_scale, post_gain):
    nc = CHUNKS
    rows, width = tokens.shape
    depth, ff = up_weight.shape
    half, dc = ff // 2, depth // nc
    blocks = 4 * nc
    bf, f32 = jnp.bfloat16, jnp.float32
    dma = pltpu.SemaphoreType.DMA
    anywhere, vmem = pl.BlockSpec(memory_space=pl.ANY), pl.BlockSpec(memory_space=pltpu.VMEM)
    return pl.pallas_call(
        functools.partial(kernel, nc),
        out_shape=jax.ShapeDtypeStruct((rows, width), bf),
        in_specs=[anywhere, anywhere, anywhere, vmem, vmem, vmem, vmem],
        out_specs=vmem,
        scratch_shapes=[
            pltpu.VMEM((rows, width), bf),
            pltpu.VMEM((depth, ff), f32),
            pltpu.VMEM((ff, depth), f32),
            pltpu.VMEM((2, width, half), bf),
            pltpu.VMEM((blocks, ff, dc), bf),
            pltpu.VMEM((2 * rows, width), bf),
            pltpu.VMEM((2 * rows, ff), bf),
            pltpu.VMEM((4, 1, depth), f32),
            pltpu.VMEM((2, rows, dc), f32),
            pltpu.VMEM((blocks, rows, dc), bf),
            pltpu.VMEM((blocks, rows, dc), bf),
            pltpu.VMEM((blocks, rows, dc), bf),
            pltpu.VMEM((blocks, rows, dc), bf),
            pltpu.VMEM((blocks, rows, dc), bf),
            pltpu.VMEM((blocks, rows, dc), bf),
            dma((64 * nc,)),
            dma((2, 4, nc, 2)),
            dma((4,)),
            dma((4,)),
            dma((blocks,)),
            dma((blocks,)),
            dma((blocks,)),
            dma((2, nc, 2)),
            dma((2,)),
        ],
        compiler_params=pltpu.CompilerParams(
            collective_id=0, has_side_effects=True, vmem_limit_bytes=60 << 20
        ),
    )(tokens, up_weight, down_weight, up_scale.reshape(1, ff), down_scale.reshape(1, depth),
      pre_gain.reshape(1, width), post_gain.reshape(1, width))


def solution(mesh):
    placed = (P(("grp", "fs"), None), P(), P("fs", "tp"), P("tp"), P("tp", "fs"), P("fs"), P())
    sizes = mesh.shape
    line = sizes["grp"] == 2 and sizes["fs"] == 4 and sizes["tp"] == 4
    return jax.shard_map(
        fused if line else plain, mesh=mesh, in_specs=placed, out_specs=P(("grp", "fs"), None), check_vma=False
    )
```
